32 devices in a mesh: sp: 8 (over z, y), tp: 4 (over x, core).
Axes of the slice: x: 2, y: 2, z: 4, core: 2. Of those that a mesh axis runs over, the one named last changes fastest.
Arguments:
- skip_stream: bfloat16 [6144, 2048], P(('sp', 'tp')), may hold values from -24 to 24
- acceptance_signal: bfloat16 [6144, 2048], P('sp', 'tp'), may hold values from -6 to 6
- lookup_mapped: bfloat16 [6144, 2048], P('sp', 'tp'), may hold values from -12 to 12
- payload_mapped: bfloat16 [6144, 2048], P('sp', 'tp'), may hold values from -6 to 6
- result_switch: bfloat16 [6144, 2048], P('sp', 'tp'), may hold values from -6 to 6
- forget_dynamic_share: bfloat16 [6144, 2048], P('sp', 'tp'), may hold values from -4 to 4
- additive_forget_logarithm: float32 [6144, 32], P('sp', 'tp'), may hold values from -1 to 0
- forget_feature_offset: float32 [2048], P('tp'), may hold values from -11 to -3
- substitution_dynamic_share: bfloat16 [6144, 2048], P('sp', 'tp'), may hold values from -6 to 6
- substitution_feature_offset: float32 [2048], P('tp'), may hold values from -6.5 to 2.5
- diagonal_reward_scales: float32 [2048], P('tp'), may hold values from -0.9 to 0.9
- result_matrix: bfloat16 [2048, 2048], P('tp'), may hold values from -0.125 to 0.125
- mlp_rescaler: float32 [2048], replicated, may hold values from 0.1 to 1.9
- switch_matrix: bfloat16 [2048, 5120], P('sp', 'tp'), may hold values from -0.125 to 0.125
- expand_matrix: bfloat16 [2048, 5120], P('sp', 'tp'), may hold values from -0.125 to 0.125
- contract_matrix: bfloat16 [2048, 5120], P('sp', 'tp'), may hold values from -0.25 to 0.25
Outputs:
- mixed_out: bfloat16 [6144, 2048], P(('sp', 'tp'))
The draws below stay inside these ranges and needn't reach their ends.
All inputs are finite; a program needn't handle non-finite values.
Results may differ from the reference program's by a relative error of at most 0.015.
Values may be sent and summed in bfloat16 or wider, within the bound.
No kernel may reach another device: no remote copies, remote signals or barrier semaphores. Data moves between devices by JAX's collectives and lax.ppermute only.
A program may use at most 128 MiB of HBM per device.

```python
import jax
import jax.numpy as jnp
from jax import lax

EMBED_DIMENSION = 2048
PER_GROUP_DIMS = 64
FF = 5120
TOK_DEV = 768
TOKENS = 6144
N_TP = 4


def draw_skip_stream(key, part):
    entries = jnp.clip(jax.random.normal(jax.random.fold_in(key, 11), (TOKENS, EMBED_DIMENSION), jnp.float32), -4.0, 4.0)
    column_scale = jnp.exp(jnp.linspace(jnp.log(0.3), jnp.log(3.0), EMBED_DIMENSION))
    row_scale = jnp.exp(jax.random.uniform(jax.random.fold_in(key, 12), (TOKENS, 1), jnp.float32, jnp.log(0.5), jnp.log(2.0)))
    return (entries * column_scale[None, :] * row_scale).astype(jnp.bfloat16)


def draw_lookup_mapped(key, part):
    attention_groups = EMBED_DIMENSION // PER_GROUP_DIMS
    direction = jnp.clip(jax.random.normal(jax.random.fold_in(key, 51), (attention_groups, PER_GROUP_DIMS), jnp.float32), -4.0, 4.0)
    noise = jnp.clip(jax.random.normal(jax.random.fold_in(key, 52), (TOKENS, attention_groups, PER_GROUP_DIMS), jnp.float32), -4.0, 4.0)
    weight = 2.0 * jnp.ones((attention_groups, 1), jnp.float32)
    shared = weight * direction
    return (noise + shared[None, :, :]).reshape(TOKENS, EMBED_DIMENSION).astype(jnp.bfloat16)


def draw_forget_dynamic_share(key, part):
    blocks = TOKENS // TOK_DEV
    offset = jax.random.uniform(jax.random.fold_in(key, 21), (blocks, 1, 1), jnp.float32, -0.7, 0.7)
    noise = jnp.clip(jax.random.normal(jax.random.fold_in(key, 22), (blocks, TOK_DEV, EMBED_DIMENSION), jnp.float32), -3.0, 3.0)
    return (noise + offset).reshape(TOKENS, EMBED_DIMENSION).astype(jnp.bfloat16)


def draw_additive_forget_logarithm(key, part):
    spots = jax.random.randint(jax.random.fold_in(key, 31), (4,), 0, TOKENS)
    struck = jnp.any(jnp.arange(TOKENS)[:, None] == spots[None, :], axis=1)
    losses = jnp.log(jax.random.uniform(jax.random.fold_in(key, 32), (TOKENS, EMBED_DIMENSION // PER_GROUP_DIMS), jnp.float32, 0.5, 0.8))
    return jnp.where(struck[:, None], losses, 0.0).astype(jnp.float32)


def draw_forget_feature_offset(key, part):
    attention_groups = EMBED_DIMENSION // PER_GROUP_DIMS
    fast_share = 0.5
    quick_heads = jax.random.uniform(jax.random.fold_in(key, 41), (attention_groups, 1), jnp.float32) < fast_share
    quick = jax.random.uniform(jax.random.fold_in(key, 42), (attention_groups, PER_GROUP_DIMS), jnp.float32, -4.5, -3.0)
    patient = jax.random.uniform(jax.random.fold_in(key, 43), (attention_groups, PER_GROUP_DIMS), jnp.float32, -11.0, -9.0)
    return jnp.where(quick_heads, quick, patient).reshape(EMBED_DIMENSION).astype(jnp.float32)


def draw_substitution_feature_offset(key, part):
    attention_groups = EMBED_DIMENSION // PER_GROUP_DIMS
    order = jax.random.permutation(jax.random.fold_in(key, 61), attention_groups)
    levels = jnp.linspace(-6.0, 2.2, attention_groups)
    jitter = jax.random.uniform(jax.random.fold_in(key, 62), (attention_groups, PER_GROUP_DIMS), jnp.float32, -0.3, 0.3)
    return (levels[order][:, None] + jitter).reshape(EMBED_DIMENSION).astype(jnp.float32)


def steps_of(key, dims, split, least, top_value):
    gain = 1.0
    for dim, shards_of in split:
        steps = jax.random.uniform(jax.random.fold_in(jax.random.fold_in(key, 6), dim), (shards_of,), jnp.float32, least / len(split), top_value / len(split))
        gain = gain * jnp.repeat(jnp.exp(steps), dims[dim] // shards_of).reshape((-1,) + (1,) * (len(dims) - 1 - dim))
    return gain


def scatter_about(key, dims, scale, limit, cuts=(), kind=jnp.bfloat16):
    values = scale * jax.random.normal(key, dims, jnp.float32)
    if cuts:
        values = values * steps_of(key, dims, cuts, -0.22, 0.18)
    return jnp.clip(values, -limit, limit).astype(kind)


def setup_inputs(seed: int = 0) -> dict:
    seeds = jax.random.split(jax.random.key(seed), 17)
    skip_stream = draw_skip_stream(jax.random.fold_in(seeds[16], 71), 0)
    acceptance_signal = scatter_about(seeds[1], (TOKENS, EMBED_DIMENSION), 1.0, 6.0, ((0, 8), (1, 4)))
    lookup_mapped = draw_lookup_mapped(jax.random.fold_in(seeds[16], 71), 0)
    payload_mapped = scatter_about(seeds[3], (TOKENS, EMBED_DIMENSION), 1.0, 6.0, ((0, 8), (1, 4)))
    result_switch = scatter_about(seeds[4], (TOKENS, EMBED_DIMENSION), 1.0, 6.0, ((0, 8), (1, 4)))
    forget_dynamic_share = draw_forget_dynamic_share(jax.random.fold_in(seeds[16], 71), 0)
    additive_forget_logarithm = draw_additive_forget_logarithm(jax.random.fold_in(seeds[16], 71), 0)
    forget_feature_offset = draw_forget_feature_offset(jax.random.fold_in(seeds[16], 71), 0)
    substitution_dynamic_share = scatter_about(seeds[8], (TOKENS, EMBED_DIMENSION), 1.0, 6.0, ((0, 8), (1, 4)))
    substitution_feature_offset = draw_substitution_feature_offset(jax.random.fold_in(seeds[16], 71), 0)
    diagonal_reward_scales = scatter_about(seeds[10], (EMBED_DIMENSION,), 0.15, 0.9, ((0, 4),), jnp.float32)
    result_matrix = scatter_about(seeds[11], (EMBED_DIMENSION, EMBED_DIMENSION), EMBED_DIMENSION ** -0.5, 0.125, ((0, 4),))
    mlp_rescaler = jnp.clip(1.0 + 0.18 * jax.random.normal(seeds[12], (EMBED_DIMENSION,), jnp.float32), 0.1, 1.9)
    switch_matrix = scatter_about(seeds[13], (EMBED_DIMENSION, FF), EMBED_DIMENSION ** -0.5, 0.125, ((0, 8), (1, 4)))
    expand_matrix = scatter_about(seeds[14], (EMBED_DIMENSION, FF), EMBED_DIMENSION ** -0.5, 0.125, ((0, 8), (1, 4)))
    contract_matrix = scatter_about(seeds[15], (EMBED_DIMENSION, FF), (FF // 8) ** -0.5, 0.25, ((0, 8), (1, 4)))
    return dict(skip_stream=skip_stream, acceptance_signal=acceptance_signal, lookup_mapped=lookup_mapped, payload_mapped=payload_mapped, result_switch=result_switch, forget_dynamic_share=forget_dynamic_share, additive_forget_logarithm=additive_forget_logarithm, forget_feature_offset=forget_feature_offset, substitution_dynamic_share=substitution_dynamic_share, substitution_feature_offset=substitution_feature_offset, diagonal_reward_scales=diagonal_reward_scales, result_matrix=result_matrix, mlp_rescaler=mlp_rescaler, switch_matrix=switch_matrix, expand_matrix=expand_matrix, contract_matrix=contract_matrix)


norm_eps = 1e-06
group_eps = 0.00064
half_step = 0.5

def group_sum(left, right, groups):
    span = left.shape[1] // groups

    def add_group(total, index):
        first = (index * span).astype(jnp.int32)
        left_part = lax.dynamic_slice_in_dim(left, first, span, 1)
        right_part = lax.dynamic_slice_in_dim(right, first, span, 0)
        partial_prod = jnp.dot(left_part, right_part, preferred_element_type=jnp.float32)
        partial_prod = lax.optimization_barrier(partial_prod.astype(jnp.bfloat16)).astype(jnp.float32)
        return (total + partial_prod, None)
    start_total = jnp.zeros((left.shape[0], right.shape[1]), jnp.float32)
    total, _ = lax.scan(add_group, start_total, jnp.arange(groups, dtype=jnp.int32))
    return total.astype(jnp.bfloat16)

def advance(memory, inputs):
    read_now, decay_now, key_now, value_now, unit_now, rate_now = inputs
    recall = lax.optimization_barrier(jnp.sum(memory * unit_now[:, None, :], axis=-1))
    memory = memory * decay_now[:, None, :] - recall[:, :, None] * (unit_now * rate_now)[:, None, :] + value_now[:, :, None] * key_now[:, None, :]
    return (memory, lax.optimization_barrier(jnp.sum(memory * read_now[:, None, :], axis=-1)))

def reference(skip_stream, acceptance_signal, lookup_mapped, payload_mapped, result_switch, forget_dynamic_share, additive_forget_logarithm, forget_feature_offset, substitution_dynamic_share, substitution_feature_offset, diagonal_reward_scales, result_matrix, mlp_rescaler, switch_matrix, expand_matrix, contract_matrix):
    sequence_span = skip_stream.shape[0]
    attention_groups = EMBED_DIMENSION // PER_GROUP_DIMS

    def by_head(values):
        return values.astype(jnp.float32).reshape(sequence_span, attention_groups, PER_GROUP_DIMS)
    acceptance_lines = by_head(acceptance_signal)
    lookup_vectors = by_head(lookup_mapped)
    payload_vectors = by_head(payload_mapped)
    log_decay_rate = -jax.nn.softplus(-(forget_feature_offset[None, :] + forget_dynamic_share.astype(jnp.float32))) - 0.5
    decay_factor_step = jnp.exp(-jnp.exp(log_decay_rate).reshape(sequence_span, attention_groups, PER_GROUP_DIMS) + additive_forget_logarithm[:, :, None])
    replace_rate = jax.nn.sigmoid(substitution_feature_offset[None, :] + substitution_dynamic_share.astype(jnp.float32))
    replace_rate = replace_rate.reshape(sequence_span, attention_groups, PER_GROUP_DIMS)
    unit_key = lookup_vectors * lax.rsqrt(lax.optimization_barrier(jnp.sum(lookup_vectors * lookup_vectors, axis=-1, keepdims=True)) + norm_eps)
    start_memory = jnp.zeros((attention_groups, PER_GROUP_DIMS, PER_GROUP_DIMS), jnp.float32)
    _, outcome = lax.scan(advance, start_memory, (acceptance_lines, decay_factor_step, lookup_vectors, payload_vectors, unit_key, replace_rate))
    centre = lax.optimization_barrier(jnp.mean(outcome, axis=-1, keepdims=True))
    spread = lax.optimization_barrier(jnp.mean(jnp.square(outcome - centre), axis=-1, keepdims=True))
    rescaled_attention = (outcome - centre) * lax.rsqrt(spread + group_eps)
    diagonal_reward_summand = lax.optimization_barrier(jnp.sum(acceptance_lines * lookup_vectors * diagonal_reward_scales.reshape(attention_groups, PER_GROUP_DIMS), axis=-1, keepdims=True)) * payload_vectors
    merged_attention = ((rescaled_attention + diagonal_reward_summand).reshape(sequence_span, EMBED_DIMENSION) * result_switch.astype(jnp.float32)).astype(jnp.bfloat16)
    projected = group_sum(merged_attention, result_matrix, N_TP)
    stream = skip_stream.astype(jnp.float32) + projected.astype(jnp.float32)
    scale_rows = lax.rsqrt(lax.optimization_barrier(jnp.mean(stream * stream, axis=-1, keepdims=True)) + norm_eps)
    normed_rows = (stream * scale_rows * mlp_rescaler[None, :]).astype(jnp.bfloat16)
    gate_act = jnp.dot(normed_rows, switch_matrix, preferred_element_type=jnp.float32)
    up_act = jnp.dot(normed_rows, expand_matrix, preferred_element_type=jnp.float32)
    hidden = (jax.nn.silu(gate_act) * up_act).astype(jnp.bfloat16)
    ffn_out = group_sum(hidden, contract_matrix.T, N_TP)
    return (stream + half_step * ffn_out.astype(jnp.float32)).astype(jnp.bfloat16)
```

```python
import functools

import jax
import jax.numpy as jnp
from jax import lax
from jax.experimental import pallas as pl
from jax.experimental.pallas import tpu as pltpu
from jax.sharding import PartitionSpec as P

PER_GROUP_DIMS = 64
PAIR = 2 * PER_GROUP_DIMS

norm_eps = 1e-06
group_eps = 0.00064
half_step = 0.5
exact = lax.Precision.HIGHEST
root_scale = 0.6065306597126334


def mm(left, right, dims=((1,), (0,))):
    return lax.dot_general(
        left.astype(jnp.bfloat16),
        right.astype(jnp.bfloat16),
        (dims, ((), ())),
        preferred_element_type=jnp.float32,
    )


def mm_exact(left, right):
    return lax.dot_general(
        left, right, (((1,), (0,)), ((), ())), precision=exact, preferred_element_type=jnp.float32
    )


def sigmoid(x):
    return 1.0 / (1.0 + jnp.exp(-x))


def lanes_of_first(width):
    lane = lax.broadcasted_iota(jnp.int32, (1, width), 1)
    return (lane & (PAIR - 1)) < PER_GROUP_DIMS


def spread(values):
    first = lanes_of_first(values.shape[1])
    zero = jnp.zeros_like(values)
    return jnp.concatenate([jnp.where(first, values, zero), jnp.where(first, zero, values)], axis=0)


def fold(values):
    half = values.shape[0] // 2
    return values[:half] + values[half:]


def head_ones(scale):
    row = lax.broadcasted_iota(jnp.int32, (PAIR, PAIR), 0)
    col = lax.broadcasted_iota(jnp.int32, (PAIR, PAIR), 1)
    return jnp.where((row < PER_GROUP_DIMS) == (col < PER_GROUP_DIMS), scale, 0.0).astype(jnp.float32)


def scan_kernel(
    read_ref, key_ref, value_ref, forget_ref, rate_ref, loss_ref, forget_off_ref, rate_off_ref,
    local_ref, coef_ref, final_ref, carry_ref,
):
    rows, breadth = read_ref.shape
    length = min(PER_GROUP_DIMS, rows)
    pairs = breadth // PAIR
    size = 2 * length
    row = lax.broadcasted_iota(jnp.int32, (size, size), 0)
    col = lax.broadcasted_iota(jnp.int32, (size, size), 1)
    krow = lax.broadcasted_iota(jnp.int32, (PAIR, PAIR), 0)
    kcol = lax.broadcasted_iota(jnp.int32, (PAIR, PAIR), 1)
    eye_k = krow == kcol
    eye = row == col

    for p in range(pairs):
        carry_ref[p, :, :PAIR] = jnp.zeros((PAIR, PAIR), jnp.float32)
        carry_ref[p, :, PAIR:] = jnp.where(eye_k, 1.0, 0.0).astype(jnp.float32)

    strict = col < row
    inclusive = col <= row
    trow = lax.broadcasted_iota(jnp.int32, (length, length), 0)
    tcol = lax.broadcasted_iota(jnp.int32, (length, length), 1)
    lower = jnp.where(tcol <= trow, 1.0, 0.0).astype(jnp.float32)
    ones = head_ones(1.0)
    first = lanes_of_first(PAIR)
    level_masks = []
    b = 1
    while b < length:
        level_masks.append(
            ((row ^ col) < 2 * b) & ((row & b) != 0) & ((col & b) == 0)
        )
        b *= 2

    P_ = range(pairs)

    def prepare(p, now):
        at = slice(p * PAIR, (p + 1) * PAIR)
        key = key_ref[now, at].astype(jnp.float32)
        read = read_ref[now, at].astype(jnp.float32)
        loss = jnp.where(first, loss_ref[now, 2 * p : 2 * p + 1], loss_ref[now, 2 * p + 1 : 2 * p + 2])
        logstep = loss - root_scale * sigmoid(
            forget_off_ref[:, at] + forget_ref[now, at].astype(jnp.float32)
        )
        rate = sigmoid(rate_off_ref[:, at] + rate_ref[now, at].astype(jnp.float32))
        unit = key * lax.rsqrt(mm_exact(key * key, ones) + norm_eps)
        cum = mm_exact(lower, logstep)
        middle = cum[length // 2 - 1 : length // 2, :]
        last = cum[length - 1 : length, :]
        grow = jnp.exp(cum - middle)
        shrink = jnp.exp(middle - cum)
        before = jnp.exp(cum - logstep - middle) * unit
        from_middle = jnp.exp(middle)
        to_end = jnp.exp(last - middle)
        key_back = key * shrink
        erase_back = unit * rate * shrink
        read_fwd = read * grow
        bf = lambda a: spread(a.astype(jnp.bfloat16))
        end_col = jnp.sum(jnp.where(eye_k, jnp.exp(last), 0.0), axis=1, keepdims=True)
        return dict(
            left=jnp.concatenate([bf(before), bf(read_fwd)], axis=0),
            right=jnp.concatenate([bf(key_back), bf(erase_back)], axis=0),
            start=jnp.concatenate([bf(before * from_middle), bf(read_fwd * from_middle)], axis=0),
            ends=jnp.concatenate([bf(key_back * to_end), bf(-(erase_back * to_end))], axis=0),
            value=spread(value_ref[now, at]),
            end_col=end_col,
        )

    def one_block(turn, _):
        now = pl.ds(turn * length, length)
        prep = [prepare(p, now) for p in P_]
        grams = [mm(d["left"], d["right"], ((1,), (1,))) for d in prep]
        erase = [jnp.where(strict, g[:size, size:], 0.0) for g in grams]
        inverse = [jnp.where(eye, 1.0, jnp.where(level_masks[0], -a, 0.0)) for a in erase]
        for mask in level_masks[1:]:
            part = [mm(jnp.where(mask, a, 0.0), x) for a, x in zip(erase, inverse)]
            inverse = [x - mm(x, y) for x, y in zip(inverse, part)]
        within = [
            mm(
                jnp.concatenate(
                    [jnp.where(strict, g[:size, :size], 0.0), jnp.where(inclusive, g[size:, :size], 0.0)],
                    axis=0,
                ),
                d["value"],
            )
            for g, d in zip(grams, prep)
        ]
        erase_read = [jnp.where(inclusive, g[size:, size:], 0.0) for g in grams]
        carry = [carry_ref[p] for p in P_]
        from_state = [mm(d["start"], z) for d, z in zip(prep, carry)]
        pad = lambda a: jnp.concatenate([a, jnp.zeros_like(a)], axis=1)
        recalled = [
            mm(x, f[:size] + pad(w[:size])) for x, f, w in zip(inverse, from_state, within)
        ]
        outs = [
            f[size:] + pad(w[size:]) - mm(e, r)
            for f, w, e, r in zip(from_state, within, erase_read, recalled)
        ]
        for p in P_:
            d = prep[p]
            stacked = jnp.concatenate(
                [pad(d["value"]), recalled[p].astype(jnp.bfloat16)], axis=0
            )
            carry_ref[p] = d["end_col"] * carry[p] + mm(d["ends"], stacked, ((0,), (0,)))
            out = fold(outs[p])
            at = slice(p * PAIR, (p + 1) * PAIR)
            local_ref[now, at] = out[:, :PAIR]
            coef_ref[now, at] = out[:, PAIR:].astype(coef_ref.dtype)
        return 0

    lax.fori_loop(0, rows // length, one_block, 0)
    for p in P_:
        final_ref[p] = fold(carry_ref[p])


def local_scan(read, key, value, forget, rate, loss, forget_off, rate_off):
    rows, breadth = read.shape
    pairs = breadth // PAIR
    return pl.pallas_call(
        scan_kernel,
        out_shape=[
            jax.ShapeDtypeStruct((rows, breadth), jnp.float32),
            jax.ShapeDtypeStruct((rows, breadth), jnp.bfloat16),
            jax.ShapeDtypeStruct((pairs, PER_GROUP_DIMS, 2 * PAIR), jnp.float32),
        ],
        scratch_shapes=[pltpu.VMEM((pairs, PAIR, 2 * PAIR), jnp.float32)],
        name="local_scan",
    )(read, key, value, forget, rate, loss, forget_off[None, :], rate_off[None, :])


def join_kernel(earlier_ref, later_ref, out_ref, sent_ref):
    for p in range(later_ref.shape[0]):
        later = later_ref[p]
        moved = mm(spread(later[:, PAIR:]), spread(earlier_ref[p]))
        total = fold(moved) + jnp.concatenate(
            [later[:, :PAIR], jnp.zeros_like(later[:, :PAIR])], axis=1
        )
        out_ref[p] = total
        sent_ref[p] = total.astype(sent_ref.dtype)


def prefix(own, axis, count):
    def shifted(values, by):
        return lax.ppermute(values, axis, [(i, i + by) for i in range(count - by)])

    sent = shifted(own.astype(jnp.bfloat16), 1)
    held = sent.astype(jnp.float32)
    by = 1
    while by < count - 1:
        held, sent = pl.pallas_call(
            join_kernel,
            out_shape=[
                jax.ShapeDtypeStruct(own.shape, jnp.float32),
                jax.ShapeDtypeStruct(own.shape, jnp.bfloat16),
            ],
            name="join",
        )(shifted(sent, by), held)
        by *= 2
    return held


def finish_kernel(
    local_ref, coef_ref, carried_ref, read_ref, key_ref, value_ref, gate_ref, reward_ref, out_ref
):
    mean_of = head_ones(1.0 / PER_GROUP_DIMS)
    sum_of = head_ones(1.0)
    for p in range(local_ref.shape[1] // PAIR):
        at = slice(p * PAIR, (p + 1) * PAIR)
        outcome = local_ref[:, at] + mm(coef_ref[:, at], spread(carried_ref[p][:, :PAIR]))
        centred = outcome - mm_exact(outcome, mean_of)
        variance = mm_exact(centred * centred, mean_of)
        normed = centred * lax.rsqrt(variance + group_eps)
        reads = read_ref[:, at].astype(jnp.float32) * key_ref[:, at].astype(jnp.float32)
        bonus = mm_exact(reads * reward_ref[:, at], sum_of) * value_ref[:, at].astype(jnp.float32)
        out_ref[:, at] = ((normed + bonus) * gate_ref[:, at].astype(jnp.float32)).astype(out_ref.dtype)


def finish(local, coef, carried, read, key, value, gate, reward):
    rows, breadth = local.shape
    block = min(128, rows)
    wide = pl.BlockSpec((block, breadth), lambda i: (i, 0))
    return pl.pallas_call(
        finish_kernel,
        grid=(rows // block,),
        in_specs=[wide, wide, pl.BlockSpec(carried.shape, lambda i: (0, 0, 0))]
        + [wide] * 4
        + [pl.BlockSpec((1, breadth), lambda i: (0, 0))],
        out_specs=wide,
        out_shape=jax.ShapeDtypeStruct((rows, breadth), jnp.bfloat16),
        name="finish",
    )(local, coef, carried, read, key, value, gate, reward[None, :])


def per_device(
    sp_count,
    skip_stream,
    acceptance_signal,
    lookup_mapped,
    payload_mapped,
    result_switch,
    forget_dynamic_share,
    additive_forget_logarithm,
    forget_feature_offset,
    substitution_dynamic_share,
    substitution_feature_offset,
    diagonal_reward_scales,
    result_matrix,
    mlp_rescaler,
    switch_matrix,
    expand_matrix,
    contract_matrix,
):
    gate_whole, up_whole, down_whole = (
        lax.all_gather(switch_matrix, "sp", axis=0, tiled=True),
        lax.all_gather(expand_matrix, "sp", axis=0, tiled=True),
        lax.all_gather(contract_matrix, "sp", axis=0, tiled=True),
    )

    local, coef, final = local_scan(
        acceptance_signal,
        lookup_mapped,
        payload_mapped,
        forget_dynamic_share,
        substitution_dynamic_share,
        additive_forget_logarithm,
        forget_feature_offset,
        substitution_feature_offset,
    )
    carried = prefix(final, "sp", sp_count)
    local, gate_whole = lax.optimization_barrier((local, gate_whole))
    merged_attention = finish(
        local,
        coef,
        carried,
        acceptance_signal,
        lookup_mapped,
        payload_mapped,
        result_switch,
        diagonal_reward_scales,
    )
    row_block = merged_attention
    projected = lax.psum_scatter(
        jnp.dot(row_block, result_matrix, preferred_element_type=jnp.float32).astype(jnp.bfloat16),
        "tp",
        scatter_dimension=0,
        tiled=True,
    )
    stream = skip_stream.astype(jnp.float32) + lax.optimization_barrier(projected).astype(
        jnp.float32
    )
    scale_rows = lax.rsqrt(jnp.mean(stream * stream, axis=-1, keepdims=True) + norm_eps)
    normed_rows = (stream * scale_rows * mlp_rescaler[None, :]).astype(jnp.bfloat16)
    whole_rows = lax.all_gather(normed_rows, "tp", axis=0, tiled=True)
    gate_act = jnp.dot(whole_rows, gate_whole, preferred_element_type=jnp.float32)
    up_act = jnp.dot(whole_rows, up_whole, preferred_element_type=jnp.float32)
    hidden = (jax.nn.silu(gate_act) * up_act).astype(jnp.bfloat16)
    row_block = hidden
    ffn_out = lax.psum_scatter(
        lax.dot_general(
            row_block, down_whole, (((1,), (1,)), ((), ())), preferred_element_type=jnp.float32
        ).astype(jnp.bfloat16),
        "tp",
        scatter_dimension=0,
        tiled=True,
    )
    return (stream + half_step * lax.optimization_barrier(ffn_out).astype(jnp.float32)).astype(
        jnp.bfloat16
    )


def solution(mesh):
    placed = (
        P(("sp", "tp"), None),
        P("sp", "tp"),
        P("sp", "tp"),
        P("sp", "tp"),
        P("sp", "tp"),
        P("sp", "tp"),
        P("sp", "tp"),
        P("tp"),
        P("sp", "tp"),
        P("tp"),
        P("tp"),
        P("tp", None),
        P(),
        P("sp", "tp"),
        P("sp", "tp"),
        P("sp", "tp"),
    )
    return jax.shard_map(
        functools.partial(per_device, mesh.shape["sp"]), mesh=mesh, in_specs=placed, out_specs=P(("sp", "tp"), None), check_vma=False
    )
```
